32 devices in a mesh: fs: 8 (over z, core), tp: 4 (over y, x).
Axes of the slice: x: 2, y: 2, z: 4, core: 2. Of those that a mesh axis runs over, the one named last changes fastest.
Arguments:
- rows_later: bfloat16 [6144, 2048], P('fs'), may hold values from -6 to 6
- rows_earlier: bfloat16 [6144, 2048], P('fs'), may hold values from -6 to 6
- out_cotangent: bfloat16 [6144, 4096], P('fs', 'tp'), may hold values from -6 to 6
- gate_proj: bfloat16 [2048, 4096], P('fs', 'tp'), may hold values from -0.125 to 0.125
- up_proj: bfloat16 [2048, 4096], P('fs', 'tp'), may hold values from -0.125 to 0.125
- conv_taps: float32 [3, 4096], P(None, 'tp'), may hold values from -4 to 4
- conv_bias: float32 [4096], P('tp'), may hold values from -3 to 3
- gate_grad_sum: float32 [2048, 4096], P('fs', 'tp'), may hold values from -6 to 6
- up_grad_sum: float32 [2048, 4096], P('fs', 'tp'), may hold values from -6 to 6
- taps_grad_sum: float32 [3, 4096], P(None, 'tp'), may hold values from -6 to 6
- bias_grad_sum: float32 [4096], P('tp'), may hold values from -6 to 6
Outputs:
- hidden_later: bfloat16 [6144, 4096], P('fs', 'tp')
- input_grad: bfloat16 [6144, 2048], P('fs')
- gate_grad_out: float32 [2048, 4096], P('fs', 'tp')
- up_grad_out: float32 [2048, 4096], P('fs', 'tp')
- taps_grad_out: float32 [3, 4096], P(None, 'tp')
- bias_grad_out: float32 [4096], P('tp')
The draws below stay inside these ranges and needn't reach their ends.
All inputs are finite; a program needn't handle non-finite values.
Results may differ from the reference program's by a relative error of at most 0.019.
Values may be sent and summed in bfloat16 or wider, within the bound.
A program may use at most 128 MiB of HBM per device.

```python
import jax
import jax.numpy as jnp
from jax import lax

D = 2048
FF = 4096
TAPS = 3
TOK_DEV = 768
TOKENS = 6144
N_FS = 8
N_TP = 4


def raised(result, rng, source, target, shards_of, factor):
    owner, partner = [(jnp.arange(result.shape[dim]) // (result.shape[dim] // shards_of)).reshape([-1 if axis == dim else 1 for axis in range(result.ndim)]) for dim in (source, target)]
    chosen = jax.random.permutation(rng, shards_of)[partner]
    strong = (owner == chosen) | (owner == (partner + shards_of // 2) % shards_of)
    return jnp.where(strong, factor * result, result)


def shard_levels(own_key, dims, pieces, low, top_value):
    loudness = 1.0
    for axis_at, shards_of in pieces:
        heights = jax.random.uniform(jax.random.fold_in(jax.random.fold_in(own_key, 6), axis_at), (shards_of,), jnp.float32, low / len(pieces), top_value / len(pieces))
        loudness = loudness * jnp.repeat(jnp.exp(heights), dims[axis_at] // shards_of).reshape((-1,) + (1,) * (len(dims) - 1 - axis_at))
    return loudness


def scatter_about(stream_key, dims, spread, limit, shards=(), kind=jnp.bfloat16):
    values = jax.random.normal(stream_key, dims, jnp.float32) * spread
    if len(shards) > 0:
        values = shard_levels(stream_key, dims, shards, -0.22, 0.18) * values
    return jnp.clip(values, min=-limit, max=limit).astype(kind)


def heavy_noise(own_key, shape, width, reach, pieces, heavy, dtype=jnp.bfloat16):
    result = width * jax.random.normal(own_key, shape, jnp.float32)
    if pieces:
        result = result * shard_levels(own_key, shape, pieces, -0.22, 0.18)
    return jnp.clip(raised(result, jax.random.fold_in(own_key, 3), *heavy), -reach, reach).astype(dtype)


def setup_inputs(seed: int = 0) -> dict:
    key_of = jax.random.split(jax.random.key(seed), 12)
    return {
        "rows_later": scatter_about(key_of[0], (TOKENS, D), 1.0, 6.0, ((0, 8),)),
        "rows_earlier": heavy_noise(key_of[1], (TOKENS, D), 1.0, 6.0, ((0, 8),), (0, 1, 8, 2.0)),
        "out_cotangent": heavy_noise(key_of[2], (TOKENS, FF), 1.0, 6.0, ((0, 8), (1, 4)), (0, 1, 8, 2.0)),
        "gate_proj": scatter_about(key_of[3], (D, FF), D ** -0.5, 0.125, ((0, 8), (1, 4))),
        "up_proj": scatter_about(key_of[4], (D, FF), D ** -0.5, 0.125, ((0, 8), (1, 4))),
        "conv_taps": scatter_about(key_of[5], (TAPS, FF), 0.6, 4.0, ((1, 4),), jnp.float32),
        "conv_bias": scatter_about(key_of[6], (FF,), 0.5, 3.0, ((0, 4),), jnp.float32),
        "gate_grad_sum": scatter_about(key_of[7], (D, FF), 1.0, 6.0, ((0, 8), (1, 4)), jnp.float32),
        "up_grad_sum": scatter_about(key_of[8], (D, FF), 1.0, 6.0, ((0, 8), (1, 4)), jnp.float32),
        "taps_grad_sum": scatter_about(key_of[9], (TAPS, FF), 1.0, 6.0, ((1, 4),), jnp.float32),
        "bias_grad_sum": scatter_about(key_of[10], (FF,), 1.0, 6.0, ((0, 4),), jnp.float32),
    }


def shift_down(values, distance):
    total_len = values.shape[1]
    return jnp.pad(values, ((0, 0), (distance, 0), (0, 0)))[:, :total_len]

def shift_up(values, distance):
    return jnp.pad(values, ((0, 0), (0, distance), (0, 0)))[:, distance:]

def causal_mix(pre_values, conv_taps, conv_bias):
    return conv_taps[0] * shift_down(pre_values, 2) + conv_taps[1] * shift_down(pre_values, 1) + conv_taps[2] * pre_values + conv_bias

def mix_adjoint(mixed_grad, conv_taps):
    return conv_taps[2] * mixed_grad + conv_taps[1] * shift_up(mixed_grad, 1) + conv_taps[0] * shift_up(mixed_grad, 2)

def reference(rows_later, rows_earlier, out_cotangent, gate_proj, up_proj, conv_taps, conv_bias, gate_grad_sum, up_grad_sum, taps_grad_sum, bias_grad_sum):
    stacked_rows = jnp.concatenate([rows_later, rows_earlier], axis=0)
    gate_pre = jnp.dot(stacked_rows, gate_proj, preferred_element_type=jnp.float32).astype(jnp.bfloat16)
    up_value = jnp.dot(stacked_rows, up_proj, preferred_element_type=jnp.float32).astype(jnp.bfloat16)
    gate_pre, up_value = lax.optimization_barrier((gate_pre, up_value))
    gate_float = gate_pre.astype(jnp.float32).reshape(2 * N_FS, TOK_DEV, FF)
    up_float = up_value.astype(jnp.float32).reshape(2 * N_FS, TOK_DEV, FF)
    mixed = causal_mix(gate_float, conv_taps, conv_bias)
    sig_all = jax.nn.sigmoid(mixed)
    activated = mixed * sig_all
    hidden = (activated * up_float).astype(jnp.bfloat16)
    hidden_later = hidden[:N_FS].reshape(TOKENS, FF)
    cotangent = out_cotangent.astype(jnp.float32).reshape(N_FS, TOK_DEV, FF)
    mixed_back = mixed[N_FS:]
    sig_back = sig_all[N_FS:]
    up_grad = (cotangent * activated[N_FS:]).astype(jnp.bfloat16).reshape(TOKENS, FF)
    mixed_grad = cotangent * up_float[N_FS:] * sig_back * (1.0 + mixed_back * (1.0 - sig_back))
    gate_grad = mix_adjoint(mixed_grad, conv_taps).astype(jnp.bfloat16).reshape(TOKENS, FF)
    block_width = FF // N_TP
    total = jnp.zeros((TOKENS, D), jnp.float32)
    for block_index in range(N_TP):
        column_start = block_index * block_width
        column_end = column_start + block_width
        part = jnp.dot(gate_grad[:, column_start:column_end], gate_proj[:, column_start:column_end].T, preferred_element_type=jnp.float32) + jnp.dot(up_grad[:, column_start:column_end], up_proj[:, column_start:column_end].T, preferred_element_type=jnp.float32)
        part = lax.optimization_barrier(part.astype(jnp.bfloat16))
        total = total + part.astype(jnp.float32)
    input_grad = total.astype(jnp.bfloat16)
    grad_scale = lax.rsqrt(jnp.asarray(TOKENS, jnp.float32))
    gate_grad_out = gate_grad_sum + grad_scale * jnp.dot(rows_earlier.T, gate_grad, preferred_element_type=jnp.float32)
    up_grad_out = up_grad_sum + grad_scale * jnp.dot(rows_earlier.T, up_grad, preferred_element_type=jnp.float32)
    gate_back = gate_float[N_FS:]
    tap_terms = jnp.stack([lax.optimization_barrier(jnp.sum(mixed_grad * shift_down(gate_back, 2 - tap_index), axis=(0, 1))) for tap_index in range(TAPS)])
    taps_grad_out = taps_grad_sum + grad_scale * tap_terms
    bias_grad_out = bias_grad_sum + grad_scale * lax.optimization_barrier(jnp.sum(mixed_grad, axis=(0, 1)))
    return (hidden_later, input_grad, gate_grad_out, up_grad_out, taps_grad_out, bias_grad_out)
```

```python
import functools
import math

import jax
import jax.numpy as jnp
from jax import lax
from jax.experimental import pallas as pl
from jax.experimental.pallas import tpu as pltpu
from jax.sharding import PartitionSpec as P

MESH = pl.DeviceIdType.MESH
VMEM_BYTES = 58 * 1024 * 1024


def add_parts(target, parts, block):
    width = target.shape[-1]
    block = min(block, width)

    def body(index, carry):
        columns = pl.ds(pl.multiple_of(index * block, block), block)
        total = parts[0][:, columns].astype(jnp.float32)
        for part in parts[1:]:
            total += part[:, columns].astype(jnp.float32)
        target[:, columns] = total.astype(target.dtype)
        return carry

    lax.fori_loop(0, width // block, body, 0)


def reduce_kernel(
    chips,
    side,
    gate_ref,
    up_ref,
    rows_ref,
    small_ref,
    grads_out,
    rows_out,
    small_out,
    ring,
    pair,
    first_in,
    first_sum,
    second_in,
    rows_buf,
    small_buf,
    ring_send,
    ring_recv,
    pair_send,
    pair_recv,
    first_send,
    first_recv,
    second_send,
    second_recv,
    third_send,
    third_recv,
    fourth_send,
    fourth_recv,
    small_send,
    small_recv,
):
    fs = lax.axis_index("fs")
    tp = lax.axis_index("tp")
    fs_size = 2 * chips
    z = fs // 2
    core = lax.rem(fs, 2)
    partner = z * 2 + 1 - core
    ty = tp // side
    tx = lax.rem(tp, side)
    firsts = (tx, ty)
    seconds = (ty, tx)

    def first_peer(half, k):
        peer = lax.rem(firsts[half] + k, side)
        return peer, (ty * side + peer if half == 0 else peer * side + tx)

    def second_peer(half, k):
        peer = lax.rem(seconds[half] + k, side)
        return peer, (peer * side + tx if half == 0 else ty * side + peer)

    barrier = pltpu.get_barrier_semaphore()
    for k in range(1, fs_size):
        pl.semaphore_signal(
            barrier, inc=1, device_id={"fs": lax.rem(fs + k, fs_size)}, device_id_type=MESH
        )
    for half in range(2):
        for k in range(1, side):
            pl.semaphore_signal(
                barrier, inc=1, device_id={"tp": first_peer(half, k)[1]}, device_id_type=MESH
            )
    pl.semaphore_wait(barrier, fs_size - 1 + 2 * (side - 1))

    parts = (gate_ref, up_ref)

    def pair_copy(d, half):
        return pltpu.make_async_remote_copy(
            src_ref=parts[half].at[2 * d + 1 - core],
            dst_ref=pair.at[d, half],
            send_sem=pair_send.at[d, half],
            recv_sem=pair_recv.at[d, half],
            device_id={"fs": partner},
            device_id_type=MESH,
        )

    def ring_copy(way, d, half):
        target = lax.rem(fs + (2 if way == 0 else fs_size - 2), fs_size)
        return pltpu.make_async_remote_copy(
            src_ref=ring.at[way, d, half],
            dst_ref=ring.at[way, d, half],
            send_sem=ring_send.at[way, d, half],
            recv_sem=ring_recv.at[way, d, half],
            device_id={"fs": target},
            device_id_type=MESH,
        )

    def first_copy(half, k):
        peer, device = first_peer(half, k)
        return pltpu.make_async_remote_copy(
            src_ref=rows_ref.at[half, peer],
            dst_ref=first_in.at[half, k - 1],
            send_sem=first_send.at[half, k - 1],
            recv_sem=first_recv.at[half, k - 1],
            device_id={"tp": device},
            device_id_type=MESH,
        )

    def second_copy(half, k):
        peer, device = second_peer(half, k)
        return pltpu.make_async_remote_copy(
            src_ref=first_sum.at[half, peer],
            dst_ref=second_in.at[half, k - 1],
            send_sem=second_send.at[half, k - 1],
            recv_sem=second_recv.at[half, k - 1],
            device_id={"tp": device},
            device_id_type=MESH,
        )

    def third_copy(half, k, shown):
        _, device = second_peer(half, k)
        block = rows_buf.at[half, firsts[half], shown]
        return pltpu.make_async_remote_copy(
            src_ref=block,
            dst_ref=block,
            send_sem=third_send.at[half, k - 1],
            recv_sem=third_recv.at[half, k - 1],
            device_id={"tp": device},
            device_id_type=MESH,
        )

    def fourth_copy(half, k, shown):
        _, device = first_peer(half, k)
        block = rows_buf.at[half, shown]
        return pltpu.make_async_remote_copy(
            src_ref=block,
            dst_ref=block,
            send_sem=fourth_send.at[half, k - 1],
            recv_sem=fourth_recv.at[half, k - 1],
            device_id={"tp": device},
            device_id_type=MESH,
        )

    def small_copy(k, slot):
        return pltpu.make_async_remote_copy(
            src_ref=small_ref,
            dst_ref=small_buf.at[slot],
            send_sem=small_send.at[k - 1],
            recv_sem=small_recv.at[k - 1],
            device_id={"fs": lax.rem(fs + k, fs_size)},
            device_id_type=MESH,
        )

    def start_first():
        for k in range(1, side):
            for half in range(2):
                first_copy(half, k).start()

    def start_second():
        for half in range(2):
            for k in range(1, side):
                first_copy(half, k).wait_recv()
            for j in range(side):
                add_parts(
                    first_sum.at[half, j],
                    [rows_ref.at[half, firsts[half], j]]
                    + [first_in.at[half, k, j] for k in range(side - 1)],
                    256,
                )
            for k in range(1, side):
                second_copy(half, k).start()

    def start_third():
        for half in range(2):
            for k in range(1, side):
                second_copy(half, k).wait_recv()
            add_parts(
                rows_buf.at[half, firsts[half], seconds[half]],
                [first_sum.at[half, seconds[half]]]
                + [second_in.at[half, k] for k in range(side - 1)],
                256,
            )
            for k in range(1, side):
                third_copy(half, k, seconds[half]).start()

    def start_fourth():
        for half in range(2):
            for k in range(1, side):
                third_copy(half, k, lax.rem(seconds[half] + side - k, side)).wait_recv()
            for k in range(1, side):
                fourth_copy(half, k, firsts[half]).start()

    def finish_rows():
        for half in range(2):
            for k in range(1, side):
                fourth_copy(half, k, lax.rem(firsts[half] + side - k, side)).wait_recv()
        for half in range(2):
            for i in range(side):
                for j in range(side):
                    add_parts(rows_out.at[half, i, j], [rows_buf.at[half, i, j]], 256)

    def own(d, half):
        return parts[half].at[2 * d + core]

    def push(way, d, half, first_on_line):
        pair_copy(d, half).wait_recv()
        slot = ring.at[way, d, half]

        @pl.when(first_on_line)
        def _():
            add_parts(slot, [own(d, half), pair.at[d, half]], 128)

        @pl.when(jnp.logical_not(first_on_line))
        def _():
            ring_copy(way, d, half).wait_recv()
            add_parts(slot, [own(d, half), pair.at[d, half], slot], 128)

        ring_copy(way, d, half).start()

    last = chips - 1

    def ring_step(t, half):
        if t < last:

            @pl.when(t >= z)
            def _():
                push(0, last - t + z, half, z == 0)

            @pl.when(t >= last - z)
            def _():
                push(1, t - last + z, half, z == last)

            return
        pair_copy(z, half).wait_recv()
        target = grads_out.at[half]
        base = [own(z, half), pair.at[z, half]]

        @pl.when(z > 0)
        def _():
            ring_copy(0, z, half).wait_recv()

        @pl.when(z < last)
        def _():
            ring_copy(1, z, half).wait_recv()

        @pl.when(z == 0)
        def _():
            add_parts(target, base + [ring.at[1, z, half]], 128)

        @pl.when(z == last)
        def _():
            add_parts(target, base + [ring.at[0, z, half]], 128)

        @pl.when(jnp.logical_and(z > 0, z < last))
        def _():
            add_parts(target, base + [ring.at[0, z, half], ring.at[1, z, half]], 128)

    start_first()
    order = []
    for s in range((chips + 1) // 2):
        order += [last - s] + ([s] if s != last - s else [])
    for d in order:
        for half in range(2):
            pair_copy(d, half).start()
    small_buf[fs] = small_ref[...]
    stages = {2: start_second, 3: start_third, 4: start_fourth, 5: finish_rows}
    for t in range(chips):
        for half in range(2):
            ring_step(t, half)
            if t == 0 and half == 1:
                for k in range(1, fs_size):
                    small_copy(k, fs).start()
            if 2 * t + half in stages:
                stages[2 * t + half]()

    for k in range(1, fs_size):
        small_copy(k, lax.rem(fs + fs_size - k, fs_size)).wait_recv()
    total = small_buf[0]
    for source in range(1, fs_size):
        total += small_buf[source]
    small_out[...] = total

    for half in range(2):
        for d in range(chips):
            pair_copy(d, half).wait_send()
        for k in range(1, side):
            first_copy(half, k).wait_send()
            second_copy(half, k).wait_send()
            third_copy(half, k, seconds[half]).wait_send()
            fourth_copy(half, k, firsts[half]).wait_send()
        for d in range(chips):

            @pl.when(z < d)
            def _():
                ring_copy(0, d, half).wait_send()

            @pl.when(z > d)
            def _():
                ring_copy(1, d, half).wait_send()

    for k in range(1, fs_size):
        small_copy(k, fs).wait_send()


def reduce_all(gate_part, up_part, partial_rows, small):
    fs_size = lax.axis_size("fs")
    chips = fs_size // 2
    side = math.isqrt(lax.axis_size("tp"))
    depth, width = gate_part.shape[0] // fs_size, gate_part.shape[1]
    tokens, model = partial_rows.shape
    r = tokens // (2 * side * side)
    bf16, dma = jnp.bfloat16, pltpu.SemaphoreType.DMA
    vmem = pl.BlockSpec(memory_space=pltpu.VMEM)
    rows_shape = (2, side, side, r, model)
    grads, rows, small_sum = pl.pallas_call(
        functools.partial(reduce_kernel, chips, side),
        out_shape=(
            jax.ShapeDtypeStruct((2, depth, width), jnp.float32),
            jax.ShapeDtypeStruct(rows_shape, bf16),
            jax.ShapeDtypeStruct(small.shape, jnp.float32),
        ),
        in_specs=[vmem] * 4,
        out_specs=(vmem, vmem, vmem),
        scratch_shapes=[
            pltpu.VMEM((2, chips, 2, depth, width), bf16),
            pltpu.VMEM((chips, 2, depth, width), bf16),
            pltpu.VMEM((2, side - 1, side, r, model), bf16),
            pltpu.VMEM((2, side, r, model), bf16),
            pltpu.VMEM((2, side - 1, r, model), bf16),
            pltpu.VMEM(rows_shape, bf16),
            pltpu.VMEM((fs_size,) + small.shape, jnp.float32),
            dma((2, chips, 2)),
            dma((2, chips, 2)),
            dma((chips, 2)),
            dma((chips, 2)),
        ]
        + [dma((2, side - 1))] * 8
        + [dma((fs_size - 1,))] * 2,
        compiler_params=pltpu.CompilerParams(
            collective_id=0, has_side_effects=True, vmem_limit_bytes=VMEM_BYTES
        ),
    )(
        gate_part.reshape(fs_size, depth, width),
        up_part.reshape(fs_size, depth, width),
        partial_rows.reshape(rows_shape),
        small,
    )
    return grads[0], grads[1], rows.reshape(tokens, model), small_sum


def shift_down(values, distance):
    total_len = values.shape[1]
    return jnp.pad(values, ((0, 0), (distance, 0), (0, 0)))[:, :total_len]


def shift_up(values, distance):
    return jnp.pad(values, ((0, 0), (0, distance), (0, 0)))[:, distance:]


def causal_mix(pre_values, conv_taps, conv_bias):
    return (
        conv_taps[0] * shift_down(pre_values, 2)
        + conv_taps[1] * shift_down(pre_values, 1)
        + conv_taps[2] * pre_values
        + conv_bias
    )


def mix_adjoint(mixed_grad, conv_taps):
    return (
        conv_taps[2] * mixed_grad
        + conv_taps[1] * shift_up(mixed_grad, 1)
        + conv_taps[0] * shift_up(mixed_grad, 2)
    )


def contract_last(left, right):
    return lax.dot_general(
        left, right, (((1,), (1,)), ((), ())), preferred_element_type=jnp.float32
    )


def contract_first(left, right):
    return lax.dot_general(
        left, right, (((0,), (0,)), ((), ())), preferred_element_type=jnp.float32
    )


def on_device(
    rows_later,
    rows_earlier,
    out_cotangent,
    gate_proj,
    up_proj,
    conv_taps,
    conv_bias,
    gate_grad_sum,
    up_grad_sum,
    taps_grad_sum,
    bias_grad_sum,
):
    seq_len = rows_later.shape[0]
    shard_width = out_cotangent.shape[1]
    stacked_rows = jnp.concatenate([rows_later, rows_earlier], axis=0)
    paired = jnp.stack([gate_proj, up_proj], axis=0)
    pieces = lax.all_gather(paired, "fs", axis=1, tiled=True)
    gate_acc = jnp.dot(stacked_rows, pieces[0], preferred_element_type=jnp.float32)
    up_acc = jnp.dot(stacked_rows, pieces[1], preferred_element_type=jnp.float32)
    gate_pre = gate_acc.astype(jnp.bfloat16)
    up_value = up_acc.astype(jnp.bfloat16)
    gate_pre, up_value = lax.optimization_barrier((gate_pre, up_value))
    gate_float = gate_pre.astype(jnp.float32).reshape(2, seq_len, shard_width)
    up_float = up_value.astype(jnp.float32).reshape(2, seq_len, shard_width)
    mixed = causal_mix(gate_float, conv_taps, conv_bias)
    sig_all = jax.nn.sigmoid(mixed)
    activated = mixed * sig_all
    hidden = (activated * up_float).astype(jnp.bfloat16)
    hidden_later = hidden[0]
    grad_scale = lax.rsqrt(jnp.asarray(seq_len * lax.axis_size("fs"), jnp.float32))

    def make_term(grad_rows):
        return contract_first(rows_earlier, grad_rows)

    cotangent = out_cotangent.astype(jnp.float32)[None]
    mixed_back = mixed[1:]
    sig_back = sig_all[1:]
    up_grad = (cotangent * activated[1:]).astype(jnp.bfloat16)[0]
    up_part = make_term(up_grad).astype(jnp.bfloat16)
    mixed_grad = cotangent * up_float[1:] * sig_back * (1.0 + mixed_back * (1.0 - sig_back))
    gate_grad = mix_adjoint(mixed_grad, conv_taps).astype(jnp.bfloat16)[0]
    gate_part = make_term(gate_grad).astype(jnp.bfloat16)
    partial_rows = contract_last(gate_grad, pieces[0]) + contract_last(up_grad, pieces[1])
    gate_back = gate_float[1:]
    tap_local = jnp.stack(
        [
            jnp.sum(mixed_grad * shift_down(gate_back, 2 - tap_index), axis=(0, 1))
            for tap_index in range(conv_taps.shape[0])
        ]
    )
    bias_local = jnp.sum(mixed_grad, axis=(0, 1))
    taps = conv_taps.shape[0]
    small = jnp.concatenate([tap_local, bias_local[None]], axis=0)
    small = jnp.pad(small, ((0, -(taps + 1) % 8), (0, 0)))
    gate_summed, up_summed, input_grad, small_sum = reduce_all(
        gate_part, up_part, partial_rows.astype(jnp.bfloat16), small
    )
    tap_total, bias_total = small_sum[:taps], small_sum[taps]
    gate_grad_out = gate_grad_sum + grad_scale * gate_summed
    up_grad_out = up_grad_sum + grad_scale * up_summed
    taps_grad_out = taps_grad_sum + grad_scale * tap_total
    bias_grad_out = bias_grad_sum + grad_scale * bias_total
    return (hidden_later, input_grad, gate_grad_out, up_grad_out, taps_grad_out, bias_grad_out)


def solution(mesh):
    placed = (
        P("fs", None),
        P("fs", None),
        P("fs", "tp"),
        P("fs", "tp"),
        P("fs", "tp"),
        P(None, "tp"),
        P("tp"),
        P("fs", "tp"),
        P("fs", "tp"),
        P(None, "tp"),
        P("tp"),
    )
    return jax.shard_map(
        on_device,
        mesh=mesh,
        in_specs=placed,
        out_specs=(
            P("fs", "tp"),
            P("fs", None),
            P("fs", "tp"),
            P("fs", "tp"),
            P(None, "tp"),
            P("tp"),
        ),
        check_vma=False,
    )
```

```python
import functools
import math

import jax
import jax.numpy as jnp
from jax import lax
from jax.experimental import pallas as pl
from jax.experimental.pallas import tpu as pltpu
from jax.sharding import PartitionSpec as P

MESH = pl.DeviceIdType.MESH
VMEM_BYTES = 58 * 1024 * 1024


def add_parts(target, parts, block):
    width = target.shape[-1]
    block = min(block, width)

    def body(index, carry):
        columns = pl.ds(pl.multiple_of(index * block, block), block)
        total = parts[0][:, columns].astype(jnp.float32)
        for part in parts[1:]:
            total += part[:, columns].astype(jnp.float32)
        target[:, columns] = total.astype(target.dtype)
        return carry

    lax.fori_loop(0, width // block, body, 0)


def reduce_kernel(
    chips,
    side,
    gate_ref,
    up_ref,
    rows_ref,
    small_ref,
    grads_out,
    rows_out,
    small_out,
    ring,
    pair,
    first_in,
    first_sum,
    second_in,
    rows_buf,
    small_buf,
    ring_send,
    ring_recv,
    pair_send,
    pair_recv,
    first_send,
    first_recv,
    second_send,
    second_recv,
    third_send,
    third_recv,
    fourth_send,
    fourth_recv,
    small_send,
    small_recv,
):
    fs = lax.axis_index("fs")
    tp = lax.axis_index("tp")
    fs_size = 2 * chips
    z = fs // 2
    core = lax.rem(fs, 2)
    partner = z * 2 + 1 - core
    ty = tp // side
    tx = lax.rem(tp, side)
    firsts = (tx, ty)
    seconds = (ty, tx)

    def first_peer(half, k):
        peer = lax.rem(firsts[half] + k, side)
        return peer, (ty * side + peer if half == 0 else peer * side + tx)

    def second_peer(half, k):
        peer = lax.rem(seconds[half] + k, side)
        return peer, (peer * side + tx if half == 0 else ty * side + peer)

    barrier = pltpu.get_barrier_semaphore()
    for k in range(1, fs_size):
        pl.semaphore_signal(
            barrier, inc=1, device_id={"fs": lax.rem(fs + k, fs_size)}, device_id_type=MESH
        )
    for half in range(2):
        for k in range(1, side):
            pl.semaphore_signal(
                barrier, inc=1, device_id={"tp": first_peer(half, k)[1]}, device_id_type=MESH
            )
    pl.semaphore_wait(barrier, fs_size - 1 + 2 * (side - 1))

    parts = (gate_ref, up_ref)

    def pair_copy(d, half):
        return pltpu.make_async_remote_copy(
            src_ref=parts[half].at[2 * d + 1 - core],
            dst_ref=pair.at[d, half],
            send_sem=pair_send.at[d, half],
            recv_sem=pair_recv.at[d, half],
            device_id={"fs": partner},
            device_id_type=MESH,
        )

    def ring_copy(way, d, half):
        target = lax.rem(fs + (2 if way == 0 else fs_size - 2), fs_size)
        return pltpu.make_async_remote_copy(
            src_ref=ring.at[way, d, half],
            dst_ref=ring.at[way, d, half],
            send_sem=ring_send.at[way, d, half],
            recv_sem=ring_recv.at[way, d, half],
            device_id={"fs": target},
            device_id_type=MESH,
        )

    def first_copy(half, k):
        peer, device = first_peer(half, k)
        return pltpu.make_async_remote_copy(
            src_ref=rows_ref.at[half, peer],
            dst_ref=first_in.at[half, k - 1],
            send_sem=first_send.at[half, k - 1],
            recv_sem=first_recv.at[half, k - 1],
            device_id={"tp": device},
            device_id_type=MESH,
        )

    def second_copy(half, k):
        peer, device = second_peer(half, k)
        return pltpu.make_async_remote_copy(
            src_ref=first_sum.at[half, peer],
            dst_ref=second_in.at[half, k - 1],
            send_sem=second_send.at[half, k - 1],
            recv_sem=second_recv.at[half, k - 1],
            device_id={"tp": device},
            device_id_type=MESH,
        )

    def third_copy(half, k, shown):
        _, device = second_peer(half, k)
        block = rows_buf.at[half, firsts[half], shown]
        return pltpu.make_async_remote_copy(
            src_ref=block,
            dst_ref=block,
            send_sem=third_send.at[half, k - 1],
            recv_sem=third_recv.at[half, k - 1],
            device_id={"tp": device},
            device_id_type=MESH,
        )

    def fourth_copy(half, k, shown):
        _, device = first_peer(half, k)
        block = rows_buf.at[half, shown]
        return pltpu.make_async_remote_copy(
            src_ref=block,
            dst_ref=block,
            send_sem=fourth_send.at[half, k - 1],
            recv_sem=fourth_recv.at[half, k - 1],
            device_id={"tp": device},
            device_id_type=MESH,
        )

    def small_copy(k, slot):
        return pltpu.make_async_remote_copy(
            src_ref=small_ref,
            dst_ref=small_buf.at[slot],
            send_sem=small_send.at[k - 1],
            recv_sem=small_recv.at[k - 1],
            device_id={"fs": lax.rem(fs + k, fs_size)},
            device_id_type=MESH,
        )

    def start_first():
        for k in range(1, side):
            for half in range(2):
                first_copy(half, k).start()

    def start_second():
        for half in range(2):
            for k in range(1, side):
                first_copy(half, k).wait_recv()
            for j in range(side):
                add_parts(
                    first_sum.at[half, j],
                    [rows_ref.at[half, firsts[half], j]]
                    + [first_in.at[half, k, j] for k in range(side - 1)],
                    256,
                )
            for k in range(1, side):
                second_copy(half, k).start()

    def start_third():
        for half in range(2):
            for k in range(1, side):
                second_copy(half, k).wait_recv()
            add_parts(
                rows_buf.at[half, firsts[half], seconds[half]],
                [first_sum.at[half, seconds[half]]]
                + [second_in.at[half, k] for k in range(side - 1)],
                256,
            )
            for k in range(1, side):
                third_copy(half, k, seconds[half]).start()

    def start_fourth():
        for half in range(2):
            for k in range(1, side):
                third_copy(half, k, lax.rem(seconds[half] + side - k, side)).wait_recv()
            for k in range(1, side):
                fourth_copy(half, k, firsts[half]).start()

    def finish_rows():
        for half in range(2):
            for k in range(1, side):
                fourth_copy(half, k, lax.rem(firsts[half] + side - k, side)).wait_recv()
        for half in range(2):
            for i in range(side):
                for j in range(side):
                    add_parts(rows_out.at[half, i, j], [rows_buf.at[half, i, j]], 256)

    def own(d, half):
        return parts[half].at[2 * d + core]

    def push(way, d, half, first_on_line):
        pair_copy(d, half).wait_recv()
        slot = ring.at[way, d, half]

        @pl.when(first_on_line)
        def _():
            add_parts(slot, [own(d, half), pair.at[d, half]], 128)

        @pl.when(jnp.logical_not(first_on_line))
        def _():
            ring_copy(way, d, half).wait_recv()
            add_parts(slot, [own(d, half), pair.at[d, half], slot], 128)

        ring_copy(way, d, half).start()

    last = chips - 1

    def ring_step(t, half):
        if t < last:

            @pl.when(t >= z)
            def _():
                push(0, last - t + z, half, z == 0)

            @pl.when(t >= last - z)
            def _():
                push(1, t - last + z, half, z == last)

            return
        pair_copy(z, half).wait_recv()
        target = grads_out.at[half]
        base = [own(z, half), pair.at[z, half]]

        @pl.when(z > 0)
        def _():
            ring_copy(0, z, half).wait_recv()

        @pl.when(z < last)
        def _():
            ring_copy(1, z, half).wait_recv()

        @pl.when(z == 0)
        def _():
            add_parts(target, base + [ring.at[1, z, half]], 128)

        @pl.when(z == last)
        def _():
            add_parts(target, base + [ring.at[0, z, half]], 128)

        @pl.when(jnp.logical_and(z > 0, z < last))
        def _():
            add_parts(target, base + [ring.at[0, z, half], ring.at[1, z, half]], 128)

    start_first()
    order = []
    for s in range((chips + 1) // 2):
        order += [last - s] + ([s] if s != last - s else [])
    for d in order:
        for half in range(2):
            pair_copy(d, half).start()
    small_buf[fs] = small_ref[...]
    stages = {2: start_second, 3: start_third, 4: start_fourth, 5: finish_rows}
    for t in range(chips):
        for half in range(2):
            ring_step(t, half)
            if t == 0 and half == 1:
                for k in range(1, fs_size):
                    small_copy(k, fs).start()
            if 2 * t + half in stages:
                stages[2 * t + half]()

    for k in range(1, fs_size):
        small_copy(k, lax.rem(fs + fs_size - k, fs_size)).wait_recv()
    total = small_buf[0]
    for source in range(1, fs_size):
        total += small_buf[source]
    small_out[...] = total

    for half in range(2):
        for d in range(chips):
            pair_copy(d, half).wait_send()
        for k in range(1, side):
            first_copy(half, k).wait_send()
            second_copy(half, k).wait_send()
            third_copy(half, k, seconds[half]).wait_send()
            fourth_copy(half, k, firsts[half]).wait_send()
        for d in range(chips):

            @pl.when(z < d)
            def _():
                ring_copy(0, d, half).wait_send()

            @pl.when(z > d)
            def _():
                ring_copy(1, d, half).wait_send()

    for k in range(1, fs_size):
        small_copy(k, fs).wait_send()


def reduce_all(gate_part, up_part, partial_rows, small):
    fs_size = lax.axis_size("fs")
    chips = fs_size // 2
    side = math.isqrt(lax.axis_size("tp"))
    depth, width = gate_part.shape[0] // fs_size, gate_part.shape[1]
    tokens, model = partial_rows.shape
    r = tokens // (2 * side * side)
    bf16, dma = jnp.bfloat16, pltpu.SemaphoreType.DMA
    vmem = pl.BlockSpec(memory_space=pltpu.VMEM)
    rows_shape = (2, side, side, r, model)
    grads, rows, small_sum = pl.pallas_call(
        functools.partial(reduce_kernel, chips, side),
        out_shape=(
            jax.ShapeDtypeStruct((2, depth, width), jnp.float32),
            jax.ShapeDtypeStruct(rows_shape, bf16),
            jax.ShapeDtypeStruct(small.shape, jnp.float32),
        ),
        in_specs=[vmem] * 4,
        out_specs=(vmem, vmem, vmem),
        scratch_shapes=[
            pltpu.VMEM((2, chips, 2, depth, width), bf16),
            pltpu.VMEM((chips, 2, depth, width), bf16),
            pltpu.VMEM((2, side - 1, side, r, model), bf16),
            pltpu.VMEM((2, side, r, model), bf16),
            pltpu.VMEM((2, side - 1, r, model), bf16),
            pltpu.VMEM(rows_shape, bf16),
            pltpu.VMEM((fs_size,) + small.shape, jnp.float32),
            dma((2, chips, 2)),
            dma((2, chips, 2)),
            dma((chips, 2)),
            dma((chips, 2)),
        ]
        + [dma((2, side - 1))] * 8
        + [dma((fs_size - 1,))] * 2,
        compiler_params=pltpu.CompilerParams(
            collective_id=0, has_side_effects=True, vmem_limit_bytes=VMEM_BYTES
        ),
    )(
        gate_part.reshape(fs_size, depth, width),
        up_part.reshape(fs_size, depth, width),
        partial_rows.reshape(rows_shape),
        small,
    )
    return grads[0], grads[1], rows.reshape(tokens, model), small_sum


def shift_down(values, distance):
    total_len = values.shape[1]
    return jnp.pad(values, ((0, 0), (distance, 0), (0, 0)))[:, :total_len]


def shift_up(values, distance):
    return jnp.pad(values, ((0, 0), (0, distance), (0, 0)))[:, distance:]


def causal_mix(pre_values, conv_taps, conv_bias):
    return (
        conv_taps[0] * shift_down(pre_values, 2)
        + conv_taps[1] * shift_down(pre_values, 1)
        + conv_taps[2] * pre_values
        + conv_bias
    )


def mix_adjoint(mixed_grad, conv_taps):
    return (
        conv_taps[2] * mixed_grad
        + conv_taps[1] * shift_up(mixed_grad, 1)
        + conv_taps[0] * shift_up(mixed_grad, 2)
    )


def contract_last(left, right):
    return lax.dot_general(
        left, right, (((1,), (1,)), ((), ())), preferred_element_type=jnp.float32
    )


def contract_first(left, right):
    return lax.dot_general(
        left, right, (((0,), (0,)), ((), ())), preferred_element_type=jnp.float32
    )


def gather_kernel(
    chips,
    later_ref,
    earlier_ref,
    gate_ref,
    up_ref,
    weights,
    gate_out,
    up_out,
    acc,
    own_sem,
    line_send,
    line_recv,
    pair_send,
    pair_recv,
):
    fs = lax.axis_index("fs")
    fs_size = 2 * chips
    z = fs // 2
    core = lax.rem(fs, 2)
    last = chips - 1
    depth = gate_ref.shape[0]
    tokens = later_ref.shape[0]
    block = math.gcd(tokens, 256)
    parts = (gate_ref, up_ref)
    outs = (gate_out, up_out)
    neighbours = (lax.rem(fs + 2, fs_size), lax.rem(fs + fs_size - 2, fs_size))
    partner = 2 * z + 1 - core

    barrier = pltpu.get_barrier_semaphore()
    for device in neighbours + (partner,):
        pl.semaphore_signal(barrier, inc=1, device_id={"fs": device}, device_id_type=MESH)
    pl.semaphore_wait(barrier, 3)

    def shard(d, half, which):
        return weights.at[half, d, pl.ds(pl.multiple_of(which * depth, depth), depth)]

    def own_copy(half):
        return pltpu.make_async_copy(parts[half], shard(z, half, core), own_sem.at[half])

    def line_copy(way, d, half, own):
        return pltpu.make_async_remote_copy(
            src_ref=parts[half] if own else shard(d, half, core),
            dst_ref=shard(d, half, core),
            send_sem=line_send.at[way, d, half],
            recv_sem=line_recv.at[d, half],
            device_id={"fs": neighbours[way]},
            device_id_type=MESH,
        )

    def pair_copy(d, half, own, which):
        return pltpu.make_async_remote_copy(
            src_ref=parts[half] if own else shard(d, half, which),
            dst_ref=shard(d, half, which),
            send_sem=pair_send.at[d, half],
            recv_sem=pair_recv.at[d, half],
            device_id={"fs": partner},
            device_id_type=MESH,
        )

    def multiply(d, half, first):
        columns = pl.ds(pl.multiple_of(d * 2 * depth, 2 * depth), 2 * depth)
        for micro, rows_ref in enumerate((later_ref, earlier_ref)):

            def body(index, carry):
                rows = pl.ds(pl.multiple_of(index * block, block), block)
                value = jnp.dot(
                    rows_ref[rows, columns],
                    weights[half, d],
                    preferred_element_type=jnp.float32,
                )
                if first:
                    acc[half, micro, rows] = value
                else:
                    acc[half, micro, rows] += value
                return carry

            lax.fori_loop(0, tokens // block, body, 0)

    for half in range(2):

        @pl.when(z < last)
        def _():
            line_copy(0, z, half, True).start()

        @pl.when(z > 0)
        def _():
            line_copy(1, z, half, True).start()

        pair_copy(z, half, True, core).start()
        own_copy(half).start()

    for half in range(2):
        own_copy(half).wait()
        pair_copy(z, half, True, 1 - core).wait_recv()
        multiply(z, half, True)

    def arrive(way, d, half, goes_on):
        line_copy(way, d, half, False).wait_recv()

        @pl.when(goes_on)
        def _():
            line_copy(way, d, half, False).start()

        pair_copy(d, half, False, core).start()

    def use(d, half):
        pair_copy(d, half, False, 1 - core).wait_recv()
        multiply(d, half, False)

    for s in range(1, chips):
        for half in range(2):

            @pl.when(z - s >= 0)
            def _():
                arrive(0, z - s, half, z < last)

            @pl.when(z + s <= last)
            def _():
                arrive(1, z + s, half, z > 0)

            @pl.when(z - s >= 0)
            def _():
                use(z - s, half)

            @pl.when(z + s <= last)
            def _():
                use(z + s, half)

    for half in range(2):
        for micro in range(2):

            def body(index, carry):
                rows = pl.ds(pl.multiple_of(index * block, block), block)
                outs[half][micro, rows] = acc[half, micro, rows].astype(outs[half].dtype)
                return carry

            lax.fori_loop(0, tokens // block, body, 0)

    for half in range(2):
        for d in range(chips):
            pair_copy(d, half, False, core).wait_send()

            @pl.when(jnp.logical_and(d <= z, z < last))
            def _():
                line_copy(0, d, half, False).wait_send()

            @pl.when(jnp.logical_and(d >= z, z > 0))
            def _():
                line_copy(1, d, half, False).wait_send()


def gather_multiply(rows_later, rows_earlier, gate_proj, up_proj):
    chips = lax.axis_size("fs") // 2
    tokens = rows_later.shape[0]
    depth, width = gate_proj.shape
    bf16, dma = jnp.bfloat16, pltpu.SemaphoreType.DMA
    vmem = pl.BlockSpec(memory_space=pltpu.VMEM)
    weights, gate_pre, up_value = pl.pallas_call(
        functools.partial(gather_kernel, chips),
        out_shape=(
            jax.ShapeDtypeStruct((2, chips, 2 * depth, width), bf16),
            jax.ShapeDtypeStruct((2, tokens, width), bf16),
            jax.ShapeDtypeStruct((2, tokens, width), bf16),
        ),
        in_specs=[vmem] * 4,
        out_specs=(vmem, vmem, vmem),
        scratch_shapes=[
            pltpu.VMEM((2, 2, tokens, width), jnp.float32),
            dma((2,)),
            dma((2, chips, 2)),
            dma((chips, 2)),
            dma((chips, 2)),
            dma((chips, 2)),
        ],
        compiler_params=pltpu.CompilerParams(
            collective_id=1, has_side_effects=True, vmem_limit_bytes=VMEM_BYTES
        ),
    )(rows_later, rows_earlier, gate_proj, up_proj)
    return weights.reshape(2, -1, width), gate_pre, up_value


def on_device(
    rows_later,
    rows_earlier,
    out_cotangent,
    gate_proj,
    up_proj,
    conv_taps,
    conv_bias,
    gate_grad_sum,
    up_grad_sum,
    taps_grad_sum,
    bias_grad_sum,
):
    seq_len = rows_later.shape[0]
    pieces, gate_pre, up_value = gather_multiply(rows_later, rows_earlier, gate_proj, up_proj)
    gate_float = gate_pre.astype(jnp.float32)
    up_float = up_value.astype(jnp.float32)
    mixed = causal_mix(gate_float, conv_taps, conv_bias)
    sig_all = jax.nn.sigmoid(mixed)
    activated = mixed * sig_all
    hidden = (activated * up_float).astype(jnp.bfloat16)
    hidden_later = hidden[0]
    grad_scale = lax.rsqrt(jnp.asarray(seq_len * lax.axis_size("fs"), jnp.float32))

    def make_term(grad_rows):
        return contract_first(rows_earlier, grad_rows)

    cotangent = out_cotangent.astype(jnp.float32)[None]
    mixed_back = mixed[1:]
    sig_back = sig_all[1:]
    up_grad = (cotangent * activated[1:]).astype(jnp.bfloat16)[0]
    up_part = make_term(up_grad).astype(jnp.bfloat16)
    mixed_grad = cotangent * up_float[1:] * sig_back * (1.0 + mixed_back * (1.0 - sig_back))
    gate_grad = mix_adjoint(mixed_grad, conv_taps).astype(jnp.bfloat16)[0]
    gate_part = make_term(gate_grad).astype(jnp.bfloat16)
    partial_rows = contract_last(gate_grad, pieces[0]) + contract_last(up_grad, pieces[1])
    gate_back = gate_float[1:]
    tap_local = jnp.stack(
        [
            jnp.sum(mixed_grad * shift_down(gate_back, 2 - tap_index), axis=(0, 1))
            for tap_index in range(conv_taps.shape[0])
        ]
    )
    bias_local = jnp.sum(mixed_grad, axis=(0, 1))
    taps = conv_taps.shape[0]
    small = jnp.concatenate([tap_local, bias_local[None]], axis=0)
    small = jnp.pad(small, ((0, -(taps + 1) % 8), (0, 0)))
    gate_summed, up_summed, input_grad, small_sum = reduce_all(
        gate_part, up_part, partial_rows.astype(jnp.bfloat16), small
    )
    tap_total, bias_total = small_sum[:taps], small_sum[taps]
    gate_grad_out = gate_grad_sum + grad_scale * gate_summed
    up_grad_out = up_grad_sum + grad_scale * up_summed
    taps_grad_out = taps_grad_sum + grad_scale * tap_total
    bias_grad_out = bias_grad_sum + grad_scale * bias_total
    return (hidden_later, input_grad, gate_grad_out, up_grad_out, taps_grad_out, bias_grad_out)


def solution(mesh):
    placed = (
        P("fs", None),
        P("fs", None),
        P("fs", "tp"),
        P("fs", "tp"),
        P("fs", "tp"),
        P(None, "tp"),
        P("tp"),
        P("fs", "tp"),
        P("fs", "tp"),
        P(None, "tp"),
        P("tp"),
    )
    return jax.shard_map(
        on_device,
        mesh=mesh,
        in_specs=placed,
        out_specs=(
            P("fs", "tp"),
            P("fs", None),
            P("fs", "tp"),
            P("fs", "tp"),
            P(None, "tp"),
            P("tp"),
        ),
        check_vma=False,
    )
```

```python
import functools
import math

import jax
import jax.numpy as jnp
from jax import lax
from jax.experimental import pallas as pl
from jax.experimental.pallas import tpu as pltpu
from jax.sharding import PartitionSpec as P

MESH = pl.DeviceIdType.MESH
VMEM_BYTES = 58 * 1024 * 1024


def add_parts(target, parts, block):
    width = target.shape[-1]
    block = min(block, width)

    def body(index, carry):
        columns = pl.ds(pl.multiple_of(index * block, block), block)
        total = parts[0][:, columns].astype(jnp.float32)
        for part in parts[1:]:
            total += part[:, columns].astype(jnp.float32)
        target[:, columns] = total.astype(target.dtype)
        return carry

    lax.fori_loop(0, width // block, body, 0)


def reduce_kernel(
    chips,
    side,
    earlier_ref,
    gate_grad_ref,
    up_grad_ref,
    weights_ref,
    small_ref,
    gate_out,
    up_out,
    rows_out,
    small_out,
    terms,
    rows_ref,
    ring,
    pair,
    first_in,
    first_sum,
    second_in,
    rows_buf,
    small_buf,
    ring_send,
    ring_recv,
    pair_send,
    pair_recv,
    first_send,
    first_recv,
    second_send,
    second_recv,
    third_send,
    third_recv,
    fourth_send,
    fourth_recv,
    small_send,
    small_recv,
):
    fs = lax.axis_index("fs")
    tp = lax.axis_index("tp")
    fs_size = 2 * chips
    z = fs // 2
    core = lax.rem(fs, 2)
    partner = z * 2 + 1 - core
    ty = tp // side
    tx = lax.rem(tp, side)
    firsts = (tx, ty)
    seconds = (ty, tx)

    def first_peer(half, k):
        peer = lax.rem(firsts[half] + k, side)
        return peer, (ty * side + peer if half == 0 else peer * side + tx)

    def second_peer(half, k):
        peer = lax.rem(seconds[half] + k, side)
        return peer, (peer * side + tx if half == 0 else ty * side + peer)

    barrier = pltpu.get_barrier_semaphore()
    for k in range(1, fs_size):
        pl.semaphore_signal(
            barrier, inc=1, device_id={"fs": lax.rem(fs + k, fs_size)}, device_id_type=MESH
        )
    for half in range(2):
        for k in range(1, side):
            pl.semaphore_signal(
                barrier, inc=1, device_id={"tp": first_peer(half, k)[1]}, device_id_type=MESH
            )
    pl.semaphore_wait(barrier, fs_size - 1 + 2 * (side - 1))

    parts = (terms.at[0], terms.at[1])
    grad_refs = (gate_grad_ref, up_grad_ref)
    outs = (gate_out, up_out)
    depth = terms.shape[2]
    wide = depth if depth % 128 == 0 else 2 * depth

    def make_terms(d, half):
        for piece in range(2 * depth // wide):
            start = pl.multiple_of(d * 2 * depth + piece * wide, wide)
            value = contract_first(earlier_ref[:, pl.ds(start, wide)], grad_refs[half][...])
            for index in range(wide // depth):
                rows = value[index * depth : (index + 1) * depth]
                terms[half, 2 * d + piece + index] = rows.astype(terms.dtype)

    def make_rows():
        model = weights_ref.shape[1]
        step = min(256, model)
        r = rows_ref.shape[3]

        def body(index, carry):
            columns = pl.ds(pl.multiple_of(index * step, step), step)
            value = contract_last(gate_grad_ref[...], weights_ref[0, columns])
            value += contract_last(up_grad_ref[...], weights_ref[1, columns])
            value = value.astype(rows_ref.dtype)
            for half in range(2):
                for i in range(side):
                    for j in range(side):
                        at = ((half * side + i) * side + j) * r
                        rows_ref[half, i, j, :, columns] = value[at : at + r]
            return carry

        lax.fori_loop(0, model // step, body, 0)

    def pair_copy(d, half):
        return pltpu.make_async_remote_copy(
            src_ref=parts[half].at[2 * d + 1 - core],
            dst_ref=pair.at[d, half],
            send_sem=pair_send.at[d, half],
            recv_sem=pair_recv.at[d, half],
            device_id={"fs": partner},
            device_id_type=MESH,
        )

    def ring_copy(way, d, half):
        target = lax.rem(fs + (2 if way == 0 else fs_size - 2), fs_size)
        return pltpu.make_async_remote_copy(
            src_ref=ring.at[way, d, half],
            dst_ref=ring.at[way, d, half],
            send_sem=ring_send.at[way, d, half],
            recv_sem=ring_recv.at[way, d, half],
            device_id={"fs": target},
            device_id_type=MESH,
        )

    def first_copy(half, k):
        peer, device = first_peer(half, k)
        return pltpu.make_async_remote_copy(
            src_ref=rows_ref.at[half, peer],
            dst_ref=first_in.at[half, k - 1],
            send_sem=first_send.at[half, k - 1],
            recv_sem=first_recv.at[half, k - 1],
            device_id={"tp": device},
            device_id_type=MESH,
        )

    def second_copy(half, k):
        peer, device = second_peer(half, k)
        return pltpu.make_async_remote_copy(
            src_ref=first_sum.at[half, peer],
            dst_ref=second_in.at[half, k - 1],
            send_sem=second_send.at[half, k - 1],
            recv_sem=second_recv.at[half, k - 1],
            device_id={"tp": device},
            device_id_type=MESH,
        )

    def third_copy(half, k, shown):
        _, device = second_peer(half, k)
        block = rows_buf.at[half, firsts[half], shown]
        return pltpu.make_async_remote_copy(
            src_ref=block,
            dst_ref=block,
            send_sem=third_send.at[half, k - 1],
            recv_sem=third_recv.at[half, k - 1],
            device_id={"tp": device},
            device_id_type=MESH,
        )

    def fourth_copy(half, k, shown):
        _, device = first_peer(half, k)
        block = rows_buf.at[half, shown]
        return pltpu.make_async_remote_copy(
            src_ref=block,
            dst_ref=block,
            send_sem=fourth_send.at[half, k - 1],
            recv_sem=fourth_recv.at[half, k - 1],
            device_id={"tp": device},
            device_id_type=MESH,
        )

    def small_copy(k, slot):
        return pltpu.make_async_remote_copy(
            src_ref=small_ref,
            dst_ref=small_buf.at[slot],
            send_sem=small_send.at[k - 1],
            recv_sem=small_recv.at[k - 1],
            device_id={"fs": lax.rem(fs + k, fs_size)},
            device_id_type=MESH,
        )

    def start_first():
        for k in range(1, side):
            for half in range(2):
                first_copy(half, k).start()

    def start_second():
        for half in range(2):
            for k in range(1, side):
                first_copy(half, k).wait_recv()
            for j in range(side):
                add_parts(
                    first_sum.at[half, j],
                    [rows_ref.at[half, firsts[half], j]]
                    + [first_in.at[half, k, j] for k in range(side - 1)],
                    256,
                )
            for k in range(1, side):
                second_copy(half, k).start()

    def start_third():
        for half in range(2):
            for k in range(1, side):
                second_copy(half, k).wait_recv()
            add_parts(
                rows_buf.at[half, firsts[half], seconds[half]],
                [first_sum.at[half, seconds[half]]]
                + [second_in.at[half, k] for k in range(side - 1)],
                256,
            )
            for k in range(1, side):
                third_copy(half, k, seconds[half]).start()

    def start_fourth():
        for half in range(2):
            for k in range(1, side):
                third_copy(half, k, lax.rem(seconds[half] + side - k, side)).wait_recv()
            for k in range(1, side):
                fourth_copy(half, k, firsts[half]).start()

    def finish_rows():
        for half in range(2):
            for k in range(1, side):
                fourth_copy(half, k, lax.rem(firsts[half] + side - k, side)).wait_recv()
        for half in range(2):
            for i in range(side):
                for j in range(side):
                    add_parts(rows_out.at[half, i, j], [rows_buf.at[half, i, j]], 256)

    def own(d, half):
        return parts[half].at[2 * d + core]

    def push(way, d, half, first_on_line):
        pair_copy(d, half).wait_recv()
        slot = ring.at[way, d, half]

        @pl.when(first_on_line)
        def _():
            add_parts(slot, [own(d, half), pair.at[d, half]], 128)

        @pl.when(jnp.logical_not(first_on_line))
        def _():
            ring_copy(way, d, half).wait_recv()
            add_parts(slot, [own(d, half), pair.at[d, half], slot], 128)

        ring_copy(way, d, half).start()

    last = chips - 1

    def ring_step(t, half):
        if t < last:

            @pl.when(t >= z)
            def _():
                push(0, last - t + z, half, z == 0)

            @pl.when(t >= last - z)
            def _():
                push(1, t - last + z, half, z == last)

            return
        pair_copy(z, half).wait_recv()
        target = outs[half]
        base = [own(z, half), pair.at[z, half]]

        @pl.when(z > 0)
        def _():
            ring_copy(0, z, half).wait_recv()

        @pl.when(z < last)
        def _():
            ring_copy(1, z, half).wait_recv()

        @pl.when(z == 0)
        def _():
            add_parts(target, base + [ring.at[1, z, half]], 128)

        @pl.when(z == last)
        def _():
            add_parts(target, base + [ring.at[0, z, half]], 128)

        @pl.when(jnp.logical_and(z > 0, z < last))
        def _():
            add_parts(target, base + [ring.at[0, z, half], ring.at[1, z, half]], 128)

    def in_turn(k):
        return jnp.where(z < chips // 2, last - k, k)

    for half in range(2):
        make_terms(in_turn(0), half)
        pair_copy(in_turn(0), half).start()
    small_buf[fs] = small_ref[...]
    for half in range(2):
        ring_step(0, half)
    make_rows()
    start_first()
    for k in range(1, chips):
        for half in range(2):
            make_terms(in_turn(k), half)
            pair_copy(in_turn(k), half).start()
    for k in range(1, fs_size):
        small_copy(k, fs).start()
    stages = {3: start_second, 4: start_third, 5: start_fourth, 6: finish_rows}
    for t in range(1, chips):
        for half in range(2):
            ring_step(t, half)
            if 2 * t + half in stages:
                stages[2 * t + half]()

    for k in range(1, fs_size):
        small_copy(k, lax.rem(fs + fs_size - k, fs_size)).wait_recv()
    total = small_buf[0]
    for source in range(1, fs_size):
        total += small_buf[source]
    small_out[...] = total

    for half in range(2):
        for d in range(chips):
            pair_copy(d, half).wait_send()
        for k in range(1, side):
            first_copy(half, k).wait_send()
            second_copy(half, k).wait_send()
            third_copy(half, k, seconds[half]).wait_send()
            fourth_copy(half, k, firsts[half]).wait_send()
        for d in range(chips):

            @pl.when(z < d)
            def _():
                ring_copy(0, d, half).wait_send()

            @pl.when(z > d)
            def _():
                ring_copy(1, d, half).wait_send()

    for k in range(1, fs_size):
        small_copy(k, fs).wait_send()


def reduce_all(rows_earlier, gate_grad, up_grad, weights, small):
    fs_size = lax.axis_size("fs")
    chips = fs_size // 2
    side = math.isqrt(lax.axis_size("tp"))
    tokens, model = rows_earlier.shape
    depth, width = model // fs_size, gate_grad.shape[1]
    r = tokens // (2 * side * side)
    bf16, dma = jnp.bfloat16, pltpu.SemaphoreType.DMA
    vmem = pl.BlockSpec(memory_space=pltpu.VMEM)
    rows_shape = (2, side, side, r, model)
    gate_sum, up_sum, rows, small_sum = pl.pallas_call(
        functools.partial(reduce_kernel, chips, side),
        out_shape=(
            jax.ShapeDtypeStruct((depth, width), jnp.float32),
            jax.ShapeDtypeStruct((depth, width), jnp.float32),
            jax.ShapeDtypeStruct(rows_shape, bf16),
            jax.ShapeDtypeStruct(small.shape, jnp.float32),
        ),
        in_specs=[vmem] * 5,
        out_specs=(vmem, vmem, vmem, vmem),
        scratch_shapes=[
            pltpu.VMEM((2, fs_size, depth, width), bf16),
            pltpu.VMEM(rows_shape, bf16),
            pltpu.VMEM((2, chips, 2, depth, width), bf16),
            pltpu.VMEM((chips, 2, depth, width), bf16),
            pltpu.VMEM((2, side - 1, side, r, model), bf16),
            pltpu.VMEM((2, side, r, model), bf16),
            pltpu.VMEM((2, side - 1, r, model), bf16),
            pltpu.VMEM(rows_shape, bf16),
            pltpu.VMEM((fs_size,) + small.shape, jnp.float32),
            dma((2, chips, 2)),
            dma((2, chips, 2)),
            dma((chips, 2)),
            dma((chips, 2)),
        ]
        + [dma((2, side - 1))] * 8
        + [dma((fs_size - 1,))] * 2,
        compiler_params=pltpu.CompilerParams(
            collective_id=0, has_side_effects=True, vmem_limit_bytes=VMEM_BYTES
        ),
    )(rows_earlier, gate_grad, up_grad, weights, small)
    return gate_sum, up_sum, rows.reshape(tokens, model), small_sum


def shift_down(values, distance):
    total_len = values.shape[1]
    return jnp.pad(values, ((0, 0), (distance, 0), (0, 0)))[:, :total_len]


def shift_up(values, distance):
    return jnp.pad(values, ((0, 0), (0, distance), (0, 0)))[:, distance:]


def causal_mix(pre_values, conv_taps, conv_bias):
    return (
        conv_taps[0] * shift_down(pre_values, 2)
        + conv_taps[1] * shift_down(pre_values, 1)
        + conv_taps[2] * pre_values
        + conv_bias
    )


def mix_adjoint(mixed_grad, conv_taps):
    return (
        conv_taps[2] * mixed_grad
        + conv_taps[1] * shift_up(mixed_grad, 1)
        + conv_taps[0] * shift_up(mixed_grad, 2)
    )


def contract_last(left, right):
    return lax.dot_general(
        left, right, (((1,), (1,)), ((), ())), preferred_element_type=jnp.float32
    )


def contract_first(left, right):
    return lax.dot_general(
        left, right, (((0,), (0,)), ((), ())), preferred_element_type=jnp.float32
    )


def gather_kernel(
    chips,
    later_ref,
    earlier_ref,
    gate_ref,
    up_ref,
    weights,
    gate_out,
    up_out,
    acc,
    own_sem,
    line_send,
    line_recv,
    pair_send,
    pair_recv,
):
    fs = lax.axis_index("fs")
    fs_size = 2 * chips
    z = fs // 2
    core = lax.rem(fs, 2)
    last = chips - 1
    depth = gate_ref.shape[0]
    tokens = later_ref.shape[0]
    block = math.gcd(tokens, 256)
    parts = (gate_ref, up_ref)
    outs = (gate_out, up_out)
    neighbours = (lax.rem(fs + 2, fs_size), lax.rem(fs + fs_size - 2, fs_size))
    partner = 2 * z + 1 - core

    barrier = pltpu.get_barrier_semaphore()
    for device in neighbours + (partner,):
        pl.semaphore_signal(barrier, inc=1, device_id={"fs": device}, device_id_type=MESH)
    pl.semaphore_wait(barrier, 3)

    def shard(d, half, which):
        return weights.at[half, d, pl.ds(pl.multiple_of(which * depth, depth), depth)]

    def own_copy(half):
        return pltpu.make_async_copy(parts[half], shard(z, half, core), own_sem.at[half])

    def line_copy(way, d, half, own):
        return pltpu.make_async_remote_copy(
            src_ref=parts[half] if own else shard(d, half, core),
            dst_ref=shard(d, half, core),
            send_sem=line_send.at[way, d, half],
            recv_sem=line_recv.at[d, half],
            device_id={"fs": neighbours[way]},
            device_id_type=MESH,
        )

    def pair_copy(d, half, own, which):
        return pltpu.make_async_remote_copy(
            src_ref=parts[half] if own else shard(d, half, which),
            dst_ref=shard(d, half, which),
            send_sem=pair_send.at[d, half],
            recv_sem=pair_recv.at[d, half],
            device_id={"fs": partner},
            device_id_type=MESH,
        )

    def multiply(d, half, first):
        columns = pl.ds(pl.multiple_of(d * 2 * depth, 2 * depth), 2 * depth)
        for micro, rows_ref in enumerate((later_ref, earlier_ref)):

            def body(index, carry):
                rows = pl.ds(pl.multiple_of(index * block, block), block)
                value = jnp.dot(
                    rows_ref[rows, columns],
                    weights[half, d],
                    preferred_element_type=jnp.float32,
                )
                if first:
                    acc[half, micro, rows] = value
                else:
                    acc[half, micro, rows] += value
                return carry

            lax.fori_loop(0, tokens // block, body, 0)

    for half in range(2):

        @pl.when(z < last)
        def _():
            line_copy(0, z, half, True).start()

        @pl.when(z > 0)
        def _():
            line_copy(1, z, half, True).start()

        pair_copy(z, half, True, core).start()
        own_copy(half).start()

    for half in range(2):
        own_copy(half).wait()
        pair_copy(z, half, True, 1 - core).wait_recv()
        multiply(z, half, True)

    def arrive(way, d, half, goes_on):
        line_copy(way, d, half, False).wait_recv()

        @pl.when(goes_on)
        def _():
            line_copy(way, d, half, False).start()

        pair_copy(d, half, False, core).start()

    def use(d, half):
        pair_copy(d, half, False, 1 - core).wait_recv()
        multiply(d, half, False)

    for s in range(1, chips):
        for half in range(2):

            @pl.when(z - s >= 0)
            def _():
                arrive(0, z - s, half, z < last)

            @pl.when(z + s <= last)
            def _():
                arrive(1, z + s, half, z > 0)

            @pl.when(z - s >= 0)
            def _():
                use(z - s, half)

            @pl.when(z + s <= last)
            def _():
                use(z + s, half)

    for half in range(2):
        for micro in range(2):

            def body(index, carry):
                rows = pl.ds(pl.multiple_of(index * block, block), block)
                outs[half][micro, rows] = acc[half, micro, rows].astype(outs[half].dtype)
                return carry

            lax.fori_loop(0, tokens // block, body, 0)

    for half in range(2):
        for d in range(chips):
            pair_copy(d, half, False, core).wait_send()

            @pl.when(jnp.logical_and(d <= z, z < last))
            def _():
                line_copy(0, d, half, False).wait_send()

            @pl.when(jnp.logical_and(d >= z, z > 0))
            def _():
                line_copy(1, d, half, False).wait_send()


def gather_multiply(rows_later, rows_earlier, gate_proj, up_proj):
    chips = lax.axis_size("fs") // 2
    tokens = rows_later.shape[0]
    depth, width = gate_proj.shape
    bf16, dma = jnp.bfloat16, pltpu.SemaphoreType.DMA
    vmem = pl.BlockSpec(memory_space=pltpu.VMEM)
    weights, gate_pre, up_value = pl.pallas_call(
        functools.partial(gather_kernel, chips),
        out_shape=(
            jax.ShapeDtypeStruct((2, chips, 2 * depth, width), bf16),
            jax.ShapeDtypeStruct((2, tokens, width), bf16),
            jax.ShapeDtypeStruct((2, tokens, width), bf16),
        ),
        in_specs=[vmem] * 4,
        out_specs=(vmem, vmem, vmem),
        scratch_shapes=[
            pltpu.VMEM((2, 2, tokens, width), jnp.float32),
            dma((2,)),
            dma((2, chips, 2)),
            dma((chips, 2)),
            dma((chips, 2)),
            dma((chips, 2)),
        ],
        compiler_params=pltpu.CompilerParams(
            collective_id=1, has_side_effects=True, vmem_limit_bytes=VMEM_BYTES
        ),
    )(rows_later, rows_earlier, gate_proj, up_proj)
    return weights.reshape(2, -1, width), gate_pre, up_value


def on_device(
    rows_later,
    rows_earlier,
    out_cotangent,
    gate_proj,
    up_proj,
    conv_taps,
    conv_bias,
    gate_grad_sum,
    up_grad_sum,
    taps_grad_sum,
    bias_grad_sum,
):
    seq_len = rows_later.shape[0]
    pieces, gate_pre, up_value = gather_multiply(rows_later, rows_earlier, gate_proj, up_proj)
    gate_float = gate_pre.astype(jnp.float32)
    up_float = up_value.astype(jnp.float32)
    mixed = causal_mix(gate_float, conv_taps, conv_bias)
    sig_all = jax.nn.sigmoid(mixed)
    activated = mixed * sig_all
    hidden = (activated * up_float).astype(jnp.bfloat16)
    hidden_later = hidden[0]
    grad_scale = lax.rsqrt(jnp.asarray(seq_len * lax.axis_size("fs"), jnp.float32))

    cotangent = out_cotangent.astype(jnp.float32)[None]
    mixed_back = mixed[1:]
    sig_back = sig_all[1:]
    up_grad = (cotangent * activated[1:]).astype(jnp.bfloat16)[0]
    mixed_grad = cotangent * up_float[1:] * sig_back * (1.0 + mixed_back * (1.0 - sig_back))
    gate_grad = mix_adjoint(mixed_grad, conv_taps).astype(jnp.bfloat16)[0]
    gate_back = gate_float[1:]
    tap_local = jnp.stack(
        [
            jnp.sum(mixed_grad * shift_down(gate_back, 2 - tap_index), axis=(0, 1))
            for tap_index in range(conv_taps.shape[0])
        ]
    )
    bias_local = jnp.sum(mixed_grad, axis=(0, 1))
    taps = conv_taps.shape[0]
    small = jnp.concatenate([tap_local, bias_local[None]], axis=0)
    small = jnp.pad(small, ((0, -(taps + 1) % 8), (0, 0)))
    gate_summed, up_summed, input_grad, small_sum = reduce_all(
        rows_earlier, gate_grad, up_grad, pieces, small
    )
    tap_total, bias_total = small_sum[:taps], small_sum[taps]
    gate_grad_out = gate_grad_sum + grad_scale * gate_summed
    up_grad_out = up_grad_sum + grad_scale * up_summed
    taps_grad_out = taps_grad_sum + grad_scale * tap_total
    bias_grad_out = bias_grad_sum + grad_scale * bias_total
    return (hidden_later, input_grad, gate_grad_out, up_grad_out, taps_grad_out, bias_grad_out)


def solution(mesh):
    placed = (
        P("fs", None),
        P("fs", None),
        P("fs", "tp"),
        P("fs", "tp"),
        P("fs", "tp"),
        P(None, "tp"),
        P("tp"),
        P("fs", "tp"),
        P("fs", "tp"),
        P(None, "tp"),
        P("tp"),
    )
    return jax.shard_map(
        on_device,
        mesh=mesh,
        in_specs=placed,
        out_specs=(
            P("fs", "tp"),
            P("fs", None),
            P("fs", "tp"),
            P("fs", "tp"),
            P(None, "tp"),
            P("tp"),
        ),
        check_vma=False,
    )
```

```python
import functools
import math

import jax
import jax.numpy as jnp
from jax import lax
from jax.experimental import pallas as pl
from jax.experimental.pallas import tpu as pltpu
from jax.sharding import PartitionSpec as P

MESH = pl.DeviceIdType.MESH
VMEM_BYTES = 58 * 1024 * 1024


def add_parts(target, parts, block):
    width = target.shape[-1]
    block = min(block, width)

    def body(index, carry):
        columns = pl.ds(pl.multiple_of(index * block, block), block)
        total = parts[0][:, columns].astype(jnp.float32)
        for part in parts[1:]:
            total += part[:, columns].astype(jnp.float32)
        target[:, columns] = total.astype(target.dtype)
        return carry

    lax.fori_loop(0, width // block, body, 0)


def reduce_kernel(
    chips,
    side,
    earlier_ref,
    gate_grad_ref,
    up_grad_ref,
    weights_ref,
    small_ref,
    gate_out,
    up_out,
    rows_out,
    small_out,
    terms,
    rows_ref,
    ring,
    pair,
    first_in,
    first_sum,
    second_in,
    rows_buf,
    small_buf,
    ring_send,
    ring_recv,
    pair_send,
    pair_recv,
    first_send,
    first_recv,
    second_send,
    second_recv,
    third_send,
    third_recv,
    fourth_send,
    fourth_recv,
    small_send,
    small_recv,
):
    fs = lax.axis_index("fs")
    tp = lax.axis_index("tp")
    fs_size = 2 * chips
    z = fs // 2
    core = lax.rem(fs, 2)
    partner = z * 2 + 1 - core
    ty = tp // side
    tx = lax.rem(tp, side)
    firsts = (tx, ty)
    seconds = (ty, tx)

    def first_peer(half, k):
        peer = lax.rem(firsts[half] + k, side)
        return peer, (ty * side + peer if half == 0 else peer * side + tx)

    def second_peer(half, k):
        peer = lax.rem(seconds[half] + k, side)
        return peer, (peer * side + tx if half == 0 else ty * side + peer)

    barrier = pltpu.get_barrier_semaphore()
    for k in range(1, fs_size):
        pl.semaphore_signal(
            barrier, inc=1, device_id={"fs": lax.rem(fs + k, fs_size)}, device_id_type=MESH
        )
    for half in range(2):
        for k in range(1, side):
            pl.semaphore_signal(
                barrier, inc=1, device_id={"tp": first_peer(half, k)[1]}, device_id_type=MESH
            )
    pl.semaphore_wait(barrier, fs_size - 1 + 2 * (side - 1))

    parts = (terms.at[0], terms.at[1])
    grad_refs = (gate_grad_ref, up_grad_ref)
    outs = (gate_out, up_out)
    depth = terms.shape[2]
    wide = depth if depth % 128 == 0 else 2 * depth

    def make_terms(d, half):
        for piece in range(2 * depth // wide):
            start = pl.multiple_of(d * 2 * depth + piece * wide, wide)
            value = contract_first(earlier_ref[:, pl.ds(start, wide)], grad_refs[half][...])
            for index in range(wide // depth):
                rows = value[index * depth : (index + 1) * depth]
                terms[half, 2 * d + piece + index] = rows.astype(terms.dtype)

    def make_rows():
        model = weights_ref.shape[1]
        step = min(256, model)
        r = rows_ref.shape[3]

        def body(index, carry):
            columns = pl.ds(pl.multiple_of(index * step, step), step)
            value = contract_last(gate_grad_ref[...], weights_ref[0, columns])
            value += contract_last(up_grad_ref[...], weights_ref[1, columns])
            value = value.astype(rows_ref.dtype)
            for half in range(2):
                for i in range(side):
                    for j in range(side):
                        at = ((half * side + i) * side + j) * r
                        rows_ref[half, i, j, :, columns] = value[at : at + r]
            return carry

        lax.fori_loop(0, model // step, body, 0)

    def pair_copy(d, half):
        return pltpu.make_async_remote_copy(
            src_ref=parts[half].at[2 * d + 1 - core],
            dst_ref=pair.at[d, half],
            send_sem=pair_send.at[d, half],
            recv_sem=pair_recv.at[d, half],
            device_id={"fs": partner},
            device_id_type=MESH,
        )

    def ring_copy(way, d, half):
        target = lax.rem(fs + (2 if way == 0 else fs_size - 2), fs_size)
        return pltpu.make_async_remote_copy(
            src_ref=ring.at[way, d, half],
            dst_ref=ring.at[way, d, half],
            send_sem=ring_send.at[way, d, half],
            recv_sem=ring_recv.at[way, d, half],
            device_id={"fs": target},
            device_id_type=MESH,
        )

    def first_copy(half, k):
        peer, device = first_peer(half, k)
        return pltpu.make_async_remote_copy(
            src_ref=rows_ref.at[half, peer],
            dst_ref=first_in.at[half, k - 1],
            send_sem=first_send.at[half, k - 1],
            recv_sem=first_recv.at[half, k - 1],
            device_id={"tp": device},
            device_id_type=MESH,
        )

    def second_copy(half, k):
        peer, device = second_peer(half, k)
        return pltpu.make_async_remote_copy(
            src_ref=first_sum.at[half, peer],
            dst_ref=second_in.at[half, k - 1],
            send_sem=second_send.at[half, k - 1],
            recv_sem=second_recv.at[half, k - 1],
            device_id={"tp": device},
            device_id_type=MESH,
        )

    def third_copy(half, k, shown):
        _, device = second_peer(half, k)
        block = rows_buf.at[half, firsts[half], shown]
        return pltpu.make_async_remote_copy(
            src_ref=block,
            dst_ref=block,
            send_sem=third_send.at[half, k - 1],
            recv_sem=third_recv.at[half, k - 1],
            device_id={"tp": device},
            device_id_type=MESH,
        )

    def fourth_copy(half, k, shown):
        _, device = first_peer(half, k)
        block = rows_buf.at[half, shown]
        return pltpu.make_async_remote_copy(
            src_ref=block,
            dst_ref=block,
            send_sem=fourth_send.at[half, k - 1],
            recv_sem=fourth_recv.at[half, k - 1],
            device_id={"tp": device},
            device_id_type=MESH,
        )

    def small_copy(k, slot):
        return pltpu.make_async_remote_copy(
            src_ref=small_ref,
            dst_ref=small_buf.at[slot],
            send_sem=small_send.at[k - 1],
            recv_sem=small_recv.at[k - 1],
            device_id={"fs": lax.rem(fs + k, fs_size)},
            device_id_type=MESH,
        )

    def start_first():
        for k in range(1, side):
            for half in range(2):
                first_copy(half, k).start()

    def start_second():
        for half in range(2):
            for k in range(1, side):
                first_copy(half, k).wait_recv()
            for j in range(side):
                add_parts(
                    first_sum.at[half, j],
                    [rows_ref.at[half, firsts[half], j]]
                    + [first_in.at[half, k, j] for k in range(side - 1)],
                    256,
                )
            for k in range(1, side):
                second_copy(half, k).start()

    def start_third():
        for half in range(2):
            for k in range(1, side):
                second_copy(half, k).wait_recv()
            add_parts(
                rows_buf.at[half, firsts[half], seconds[half]],
                [first_sum.at[half, seconds[half]]]
                + [second_in.at[half, k] for k in range(side - 1)],
                256,
            )
            for k in range(1, side):
                third_copy(half, k, seconds[half]).start()

    def start_fourth():
        for half in range(2):
            for k in range(1, side):
                third_copy(half, k, lax.rem(seconds[half] + side - k, side)).wait_recv()
            for k in range(1, side):
                fourth_copy(half, k, firsts[half]).start()

    def finish_rows():
        for half in range(2):
            for k in range(1, side):
                fourth_copy(half, k, lax.rem(firsts[half] + side - k, side)).wait_recv()
        for half in range(2):
            for i in range(side):
                for j in range(side):
                    add_parts(rows_out.at[half, i, j], [rows_buf.at[half, i, j]], 256)

    def own(d, half):
        return parts[half].at[2 * d + core]

    def push(way, d, half, first_on_line):
        pair_copy(d, half).wait_recv()
        slot = ring.at[way, d, half]

        @pl.when(first_on_line)
        def _():
            add_parts(slot, [own(d, half), pair.at[d, half]], 128)

        @pl.when(jnp.logical_not(first_on_line))
        def _():
            ring_copy(way, d, half).wait_recv()
            add_parts(slot, [own(d, half), pair.at[d, half], slot], 128)

        ring_copy(way, d, half).start()

    last = chips - 1

    def ring_step(t, half):
        if t < last:

            @pl.when(t >= z)
            def _():
                push(0, last - t + z, half, z == 0)

            @pl.when(t >= last - z)
            def _():
                push(1, t - last + z, half, z == last)

            return
        pair_copy(z, half).wait_recv()
        target = outs[half]
        base = [own(z, half), pair.at[z, half]]

        @pl.when(z > 0)
        def _():
            ring_copy(0, z, half).wait_recv()

        @pl.when(z < last)
        def _():
            ring_copy(1, z, half).wait_recv()

        @pl.when(z == 0)
        def _():
            add_parts(target, base + [ring.at[1, z, half]], 128)

        @pl.when(z == last)
        def _():
            add_parts(target, base + [ring.at[0, z, half]], 128)

        @pl.when(jnp.logical_and(z > 0, z < last))
        def _():
            add_parts(target, base + [ring.at[0, z, half], ring.at[1, z, half]], 128)

    def in_turn(k):
        return jnp.where(z < chips // 2, last - k, k)

    for half in range(2):
        make_terms(in_turn(0), half)
        pair_copy(in_turn(0), half).start()
    small_buf[fs] = small_ref[...]
    for half in range(2):
        ring_step(0, half)
    make_rows()
    start_first()
    for k in range(1, chips):
        for half in range(2):
            make_terms(in_turn(k), half)
            pair_copy(in_turn(k), half).start()
    for k in range(1, fs_size):
        small_copy(k, fs).start()
    stages = {3: start_second, 4: start_third, 5: start_fourth, 6: finish_rows}
    for t in range(1, chips):
        for half in range(2):
            ring_step(t, half)
            if 2 * t + half in stages:
                stages[2 * t + half]()

    for k in range(1, fs_size):
        small_copy(k, lax.rem(fs + fs_size - k, fs_size)).wait_recv()
    total = small_buf[0]
    for source in range(1, fs_size):
        total += small_buf[source]
    small_out[...] = total

    for half in range(2):
        for d in range(chips):
            pair_copy(d, half).wait_send()
        for k in range(1, side):
            first_copy(half, k).wait_send()
            second_copy(half, k).wait_send()
            third_copy(half, k, seconds[half]).wait_send()
            fourth_copy(half, k, firsts[half]).wait_send()
        for d in range(chips):

            @pl.when(z < d)
            def _():
                ring_copy(0, d, half).wait_send()

            @pl.when(z > d)
            def _():
                ring_copy(1, d, half).wait_send()

    for k in range(1, fs_size):
        small_copy(k, fs).wait_send()


def reduce_all(rows_earlier, gate_grad, up_grad, weights, small):
    fs_size = lax.axis_size("fs")
    chips = fs_size // 2
    side = math.isqrt(lax.axis_size("tp"))
    tokens, model = rows_earlier.shape
    depth, width = model // fs_size, gate_grad.shape[1]
    r = tokens // (2 * side * side)
    bf16, dma = jnp.bfloat16, pltpu.SemaphoreType.DMA
    vmem = pl.BlockSpec(memory_space=pltpu.VMEM)
    rows_shape = (2, side, side, r, model)
    gate_sum, up_sum, rows, small_sum = pl.pallas_call(
        functools.partial(reduce_kernel, chips, side),
        out_shape=(
            jax.ShapeDtypeStruct((depth, width), jnp.float32),
            jax.ShapeDtypeStruct((depth, width), jnp.float32),
            jax.ShapeDtypeStruct(rows_shape, bf16),
            jax.ShapeDtypeStruct(small.shape, jnp.float32),
        ),
        in_specs=[vmem] * 5,
        out_specs=(vmem, vmem, vmem, vmem),
        scratch_shapes=[
            pltpu.VMEM((2, fs_size, depth, width), bf16),
            pltpu.VMEM(rows_shape, bf16),
            pltpu.VMEM((2, chips, 2, depth, width), bf16),
            pltpu.VMEM((chips, 2, depth, width), bf16),
            pltpu.VMEM((2, side - 1, side, r, model), bf16),
            pltpu.VMEM((2, side, r, model), bf16),
            pltpu.VMEM((2, side - 1, r, model), bf16),
            pltpu.VMEM(rows_shape, bf16),
            pltpu.VMEM((fs_size,) + small.shape, jnp.float32),
            dma((2, chips, 2)),
            dma((2, chips, 2)),
            dma((chips, 2)),
            dma((chips, 2)),
        ]
        + [dma((2, side - 1))] * 8
        + [dma((fs_size - 1,))] * 2,
        compiler_params=pltpu.CompilerParams(
            collective_id=0, has_side_effects=True, vmem_limit_bytes=VMEM_BYTES
        ),
    )(rows_earlier, gate_grad, up_grad, weights, small)
    return gate_sum, up_sum, rows.reshape(tokens, model), small_sum


def contract_last(left, right):
    return lax.dot_general(
        left, right, (((1,), (1,)), ((), ())), preferred_element_type=jnp.float32
    )


def contract_first(left, right):
    return lax.dot_general(
        left, right, (((0,), (0,)), ((), ())), preferred_element_type=jnp.float32
    )


def gather_kernel(
    chips,
    later_ref,
    earlier_ref,
    gate_ref,
    up_ref,
    weights,
    gate_out,
    up_out,
    acc,
    own_sem,
    line_send,
    line_recv,
    pair_send,
    pair_recv,
):
    fs = lax.axis_index("fs")
    fs_size = 2 * chips
    z = fs // 2
    core = lax.rem(fs, 2)
    last = chips - 1
    depth = gate_ref.shape[0]
    tokens = later_ref.shape[0]
    block = math.gcd(tokens, 256)
    parts = (gate_ref, up_ref)
    outs = (gate_out, up_out)
    neighbours = (lax.rem(fs + 2, fs_size), lax.rem(fs + fs_size - 2, fs_size))
    partner = 2 * z + 1 - core

    barrier = pltpu.get_barrier_semaphore()
    for device in neighbours + (partner,):
        pl.semaphore_signal(barrier, inc=1, device_id={"fs": device}, device_id_type=MESH)
    pl.semaphore_wait(barrier, 3)

    def shard(d, half, which):
        return weights.at[half, d, pl.ds(pl.multiple_of(which * depth, depth), depth)]

    def own_copy(half):
        return pltpu.make_async_copy(parts[half], shard(z, half, core), own_sem.at[half])

    def line_copy(way, d, half, own):
        return pltpu.make_async_remote_copy(
            src_ref=parts[half] if own else shard(d, half, core),
            dst_ref=shard(d, half, core),
            send_sem=line_send.at[way, d, half],
            recv_sem=line_recv.at[d, half],
            device_id={"fs": neighbours[way]},
            device_id_type=MESH,
        )

    def pair_copy(d, half, own, which):
        return pltpu.make_async_remote_copy(
            src_ref=parts[half] if own else shard(d, half, which),
            dst_ref=shard(d, half, which),
            send_sem=pair_send.at[d, half],
            recv_sem=pair_recv.at[d, half],
            device_id={"fs": partner},
            device_id_type=MESH,
        )

    def multiply(d, half, first):
        columns = pl.ds(pl.multiple_of(d * 2 * depth, 2 * depth), 2 * depth)
        for micro, rows_ref in enumerate((later_ref, earlier_ref)):

            def body(index, carry):
                rows = pl.ds(pl.multiple_of(index * block, block), block)
                value = jnp.dot(
                    rows_ref[rows, columns],
                    weights[half, d],
                    preferred_element_type=jnp.float32,
                )
                if first:
                    acc[half, micro, rows] = value
                else:
                    acc[half, micro, rows] += value
                return carry

            lax.fori_loop(0, tokens // block, body, 0)

    for half in range(2):

        @pl.when(z < last)
        def _():
            line_copy(0, z, half, True).start()

        @pl.when(z > 0)
        def _():
            line_copy(1, z, half, True).start()

        pair_copy(z, half, True, core).start()
        own_copy(half).start()

    for half in range(2):
        own_copy(half).wait()
        pair_copy(z, half, True, 1 - core).wait_recv()
        multiply(z, half, True)

    def arrive(way, d, half, goes_on):
        line_copy(way, d, half, False).wait_recv()

        @pl.when(goes_on)
        def _():
            line_copy(way, d, half, False).start()

        pair_copy(d, half, False, core).start()

    def use(d, half):
        pair_copy(d, half, False, 1 - core).wait_recv()
        multiply(d, half, False)

    for s in range(1, chips):
        for half in range(2):

            @pl.when(z - s >= 0)
            def _():
                arrive(0, z - s, half, z < last)

            @pl.when(z + s <= last)
            def _():
                arrive(1, z + s, half, z > 0)

            @pl.when(z - s >= 0)
            def _():
                use(z - s, half)

            @pl.when(z + s <= last)
            def _():
                use(z + s, half)

    for half in range(2):
        for micro in range(2):

            def body(index, carry):
                rows = pl.ds(pl.multiple_of(index * block, block), block)
                outs[half][micro, rows] = acc[half, micro, rows].astype(outs[half].dtype)
                return carry

            lax.fori_loop(0, tokens // block, body, 0)

    for half in range(2):
        for d in range(chips):
            pair_copy(d, half, False, core).wait_send()

            @pl.when(jnp.logical_and(d <= z, z < last))
            def _():
                line_copy(0, d, half, False).wait_send()

            @pl.when(jnp.logical_and(d >= z, z > 0))
            def _():
                line_copy(1, d, half, False).wait_send()


def gather_multiply(rows_later, rows_earlier, gate_proj, up_proj):
    chips = lax.axis_size("fs") // 2
    tokens = rows_later.shape[0]
    depth, width = gate_proj.shape
    bf16, dma = jnp.bfloat16, pltpu.SemaphoreType.DMA
    vmem = pl.BlockSpec(memory_space=pltpu.VMEM)
    weights, gate_pre, up_value = pl.pallas_call(
        functools.partial(gather_kernel, chips),
        out_shape=(
            jax.ShapeDtypeStruct((2, chips, 2 * depth, width), bf16),
            jax.ShapeDtypeStruct((2, tokens, width), bf16),
            jax.ShapeDtypeStruct((2, tokens, width), bf16),
        ),
        in_specs=[vmem] * 4,
        out_specs=(vmem, vmem, vmem),
        scratch_shapes=[
            pltpu.VMEM((2, 2, tokens, width), jnp.float32),
            dma((2,)),
            dma((2, chips, 2)),
            dma((chips, 2)),
            dma((chips, 2)),
            dma((chips, 2)),
        ],
        compiler_params=pltpu.CompilerParams(
            collective_id=1, has_side_effects=True, vmem_limit_bytes=VMEM_BYTES
        ),
    )(rows_later, rows_earlier, gate_proj, up_proj)
    return weights.reshape(2, -1, width), gate_pre, up_value


def middle_kernel(
    gate_ref, up_ref, cotangent_ref, taps_ref, bias_ref, hidden_out, up_out, gate_out, small_out
):
    rows, width = cotangent_ref.shape
    count = taps_ref.shape[0]
    index = lax.broadcasted_iota(jnp.int32, (rows, width), 0)

    def down(values, distance):
        if distance == 0:
            return values
        return jnp.where(index >= distance, pltpu.roll(values, distance, 0), 0.0)

    def up(values, distance):
        if distance == 0:
            return values
        moved = pltpu.roll(values, rows - distance, 0)
        return jnp.where(index < rows - distance, moved, 0.0)

    taps = [taps_ref[k : k + 1, :] for k in range(count)]
    for micro in range(2):
        gate = gate_ref[micro].astype(jnp.float32)
        value = up_ref[micro].astype(jnp.float32)
        shifted = [down(gate, count - 1 - k) for k in range(count)]
        mixed = bias_ref[...] + taps[0] * shifted[0]
        for k in range(1, count):
            mixed += taps[k] * shifted[k]
        sig = jax.nn.sigmoid(mixed)
        activated = mixed * sig
        if micro == 0:
            hidden_out[...] = (activated * value).astype(hidden_out.dtype)
            continue
        cotangent = cotangent_ref[...].astype(jnp.float32)
        up_out[...] = (cotangent * activated).astype(up_out.dtype)
        mixed_grad = cotangent * value * sig * (1.0 + mixed * (1.0 - sig))
        total = taps[count - 1] * mixed_grad
        for k in range(count - 1):
            total += taps[k] * up(mixed_grad, count - 1 - k)
        gate_out[...] = total.astype(gate_out.dtype)
        small_out[...] = jnp.zeros_like(small_out)
        for k in range(count):
            small_out[k : k + 1, :] = jnp.sum(mixed_grad * shifted[k], axis=0, keepdims=True)
        small_out[count : count + 1, :] = jnp.sum(mixed_grad, axis=0, keepdims=True)


def middle(gate_pre, up_value, out_cotangent, conv_taps, conv_bias):
    rows, width = out_cotangent.shape
    count = conv_taps.shape[0]
    small_rows = count + 1 + -(count + 1) % 8
    block = math.gcd(width, 128)

    def columns(height):
        return pl.BlockSpec((height, block), lambda i: (0, i))

    pair = pl.BlockSpec((2, rows, block), lambda i: (0, 0, i))
    return pl.pallas_call(
        middle_kernel,
        grid=(width // block,),
        out_shape=(
            jax.ShapeDtypeStruct((rows, width), jnp.bfloat16),
            jax.ShapeDtypeStruct((rows, width), jnp.bfloat16),
            jax.ShapeDtypeStruct((rows, width), jnp.bfloat16),
            jax.ShapeDtypeStruct((small_rows, width), jnp.float32),
        ),
        in_specs=[pair, pair, columns(rows), columns(count), columns(1)],
        out_specs=(columns(rows), columns(rows), columns(rows), columns(small_rows)),
    )(gate_pre, up_value, out_cotangent, conv_taps, conv_bias[None])


def on_device(
    rows_later,
    rows_earlier,
    out_cotangent,
    gate_proj,
    up_proj,
    conv_taps,
    conv_bias,
    gate_grad_sum,
    up_grad_sum,
    taps_grad_sum,
    bias_grad_sum,
):
    seq_len = rows_later.shape[0]
    pieces, gate_pre, up_value = gather_multiply(rows_later, rows_earlier, gate_proj, up_proj)
    grad_scale = lax.rsqrt(jnp.asarray(seq_len * lax.axis_size("fs"), jnp.float32))
    hidden_later, up_grad, gate_grad, small = middle(
        gate_pre, up_value, out_cotangent, conv_taps, conv_bias
    )
    taps = conv_taps.shape[0]
    gate_summed, up_summed, input_grad, small_sum = reduce_all(
        rows_earlier, gate_grad, up_grad, pieces, small
    )
    tap_total, bias_total = small_sum[:taps], small_sum[taps]
    gate_grad_out = gate_grad_sum + grad_scale * gate_summed
    up_grad_out = up_grad_sum + grad_scale * up_summed
    taps_grad_out = taps_grad_sum + grad_scale * tap_total
    bias_grad_out = bias_grad_sum + grad_scale * bias_total
    return (hidden_later, input_grad, gate_grad_out, up_grad_out, taps_grad_out, bias_grad_out)


def solution(mesh):
    placed = (
        P("fs", None),
        P("fs", None),
        P("fs", "tp"),
        P("fs", "tp"),
        P("fs", "tp"),
        P(None, "tp"),
        P("tp"),
        P("fs", "tp"),
        P("fs", "tp"),
        P(None, "tp"),
        P("tp"),
    )
    return jax.shard_map(
        on_device,
        mesh=mesh,
        in_specs=placed,
        out_specs=(
            P("fs", "tp"),
            P("fs", None),
            P("fs", "tp"),
            P("fs", "tp"),
            P(None, "tp"),
            P("tp"),
        ),
        check_vma=False,
    )
```
